32 devices in a mesh: fs: 8 (over z, y), tp: 4 (over x, core).
Axes of the slice: x: 2, y: 2, z: 4, core: 2. Of those that a mesh axis runs over, the one named last changes fastest.
Arguments:
- layer_input: bfloat16 [6144, 2048], P('fs', 'tp'), may hold values from -6 to 6
- out_cotangent: bfloat16 [6144, 2048], P('fs', 'tp'), may hold values from -6 to 6
- gate_matrix: bfloat16 [2048, 6144], P('fs', 'tp'), may hold values from -0.125 to 0.125
- up_matrix: bfloat16 [2048, 6144], P('fs', 'tp'), may hold values from -0.125 to 0.125
- down_matrix: bfloat16 [6144, 2048], P('tp', 'fs'), may hold values from -0.078125 to 0.078125
Outputs:
- input_grad: bfloat16 [6144, 2048], P('fs', 'tp')
- gate_grad: float32 [2048, 6144], P('fs', 'tp')
- up_grad: float32 [2048, 6144], P('fs', 'tp')
- down_grad: float32 [6144, 2048], P('tp', 'fs')
The draws below stay inside these ranges and needn't reach their ends.
All inputs are finite; a program needn't handle non-finite values.
Results may differ from the reference program's by a relative error of at most 0.014.
Values may be sent and summed in bfloat16 or wider, within the bound.
A program may use at most 128 MiB of HBM per device.

```python
import jax
import jax.numpy as jnp

D = 2048
FF = 6144
TOKENS = 6144
N_TP = 4


def raised(array, key, source, target, parts, factor):
    def block_of(dim):
        return (jnp.arange(array.shape[dim]) // (array.shape[dim] // parts)).reshape((-1,) + (1,) * (array.ndim - 1 - dim))

    one_side = jax.random.permutation(key, parts)[block_of(target)]
    other_side = (block_of(target) + parts // 2) % parts
    return jnp.where((block_of(source) == one_side) | (block_of(source) == other_side), factor * array, array)


def levels(stream_key, shape, split, least, largest):
    factor_of = 1.0
    for dim, shards_of in split:
        heights = jax.random.uniform(jax.random.fold_in(jax.random.fold_in(stream_key, 6), dim), (shards_of,), jnp.float32, least / len(split), largest / len(split))
        factor_of = factor_of * jnp.repeat(jnp.exp(heights), shape[dim] // shards_of).reshape((-1,) + (1,) * (len(shape) - 1 - dim))
    return factor_of


def gaussian(own_key, shape, scale, limit, split=(), kind=jnp.bfloat16):
    result = scale * jax.random.normal(own_key, shape, jnp.float32)
    if split:
        result = result * levels(own_key, shape, split, -0.22, 0.18)
    return jnp.clip(result, -limit, limit).astype(kind)


def noise_with(key, extent, spread, most, pieces, heavy, held_as=jnp.bfloat16):
    values = spread * jax.random.normal(key, extent, jnp.float32)
    if pieces:
        values = values * levels(key, extent, pieces, -0.22, 0.18)
    return jnp.clip(raised(values, jax.random.fold_in(key, 3), *heavy), -most, most).astype(held_as)


def setup_inputs(seed: int = 0) -> dict:
    key_of = jax.random.split(jax.random.key(seed), 6)
    layer_input = gaussian(key_of[0], (TOKENS, D), 1.0, 6.0, ((0, 8), (1, 4)))
    out_cotangent = noise_with(key_of[1], (TOKENS, D), 1.0, 6.0, ((0, 8), (1, 4)), (0, 1, 8, 2.0))
    gate_matrix = gaussian(key_of[2], (D, FF), D ** -0.5, 0.125, ((0, 8), (1, 4)))
    up_matrix = gaussian(key_of[3], (D, FF), D ** -0.5, 0.125, ((0, 8), (1, 4)))
    down_matrix = gaussian(key_of[4], (FF, D), FF ** -0.5, 0.078125, ((0, 4), (1, 8)))
    return dict(layer_input=layer_input, out_cotangent=out_cotangent, gate_matrix=gate_matrix, up_matrix=up_matrix, down_matrix=down_matrix)


def reference(layer_input, out_cotangent, gate_matrix, up_matrix, down_matrix):
    gate_pre = jnp.dot(layer_input, gate_matrix, preferred_element_type=jnp.float32)
    up_pre = jnp.dot(layer_input, up_matrix, preferred_element_type=jnp.float32)
    sigmoid_gate = jax.nn.sigmoid(gate_pre)
    activation = gate_pre * sigmoid_gate
    hidden = (activation * up_pre).astype(jnp.bfloat16)
    hidden_delta = jnp.dot(out_cotangent, down_matrix.T, preferred_element_type=jnp.float32)
    up_delta = (hidden_delta * activation).astype(jnp.bfloat16)
    gate_delta = (hidden_delta * up_pre * sigmoid_gate * (1.0 + gate_pre * (1.0 - sigmoid_gate))).astype(jnp.bfloat16)
    gate_grad = jnp.dot(layer_input.T, gate_delta, preferred_element_type=jnp.float32)
    up_grad = jnp.dot(layer_input.T, up_delta, preferred_element_type=jnp.float32)
    down_grad = jnp.dot(hidden.T, out_cotangent, preferred_element_type=jnp.float32)
    block_width = FF // N_TP
    summed = jnp.zeros(layer_input.shape, jnp.float32)
    for block_index in range(N_TP):
        first_col = block_index * block_width
        last_col = first_col + block_width
        partial_value = jnp.dot(gate_delta[:, first_col:last_col], gate_matrix[:, first_col:last_col].T, preferred_element_type=jnp.float32)
        partial_value = partial_value + jnp.dot(up_delta[:, first_col:last_col], up_matrix[:, first_col:last_col].T, preferred_element_type=jnp.float32)
        summed = summed + partial_value.astype(jnp.bfloat16).astype(jnp.float32)
    return summed.astype(jnp.bfloat16), gate_grad, up_grad, down_grad
```

```python
import functools

import jax
import jax.numpy as jnp
from jax import lax
from jax.experimental import pallas as pl
from jax.experimental.pallas import tpu as pltpu
from jax.sharding import PartitionSpec as P

CORES = 2
TILE = 256
STRIPS = 3

NN = ((1,), (0,))
TN = ((0,), (0,))
NT = ((1,), (1,))

GATE, UP, DOWN = range(3)


def dot(left, right, dims):
    return lax.dot_general(left, right, (dims, ((), ())), preferred_element_type=jnp.float32)


def narrow(value):
    return value.astype(jnp.bfloat16)


def wide(value):
    return value.astype(jnp.float32)


def xor(left, right, n):
    total = 0
    k = 1
    while k < n:
        total = total + k * lax.rem(lax.div(left, k) + right // k % 2, 2)
        k *= 2
    return total


def kernel(
    n_fs,
    n_tp,
    layer_input,
    out_cotangent,
    gate_matrix,
    up_matrix,
    down_matrix,
    input_grad,
    gate_grad,
    up_grad,
    down_grad,
    xg,
    w,
    ab,
    delta,
    y_out,
    y_in,
    far_in,
    near_in,
    core_in,
    dx_out,
    dx_core,
    dx_x,
    dx_z,
    local_sem,
    out_sem,
    ag_core,
    ag_near,
    ag_far,
    ag_y,
    tok_z,
    tok_x,
    tok_core,
    rs_y,
    rs_far,
    rs_near,
    rs_core,
    dx_core_sem,
    dx_x_sem,
    dx_z_sem,
):
    n_x = n_tp // CORES
    n_y = n_x
    n_z = n_fs // n_y
    per_quarter = n_fs // n_tp
    far = range(2, n_z, 2)
    tokens, part = layer_input.shape
    depth, width = gate_matrix.shape
    half = width // 2
    model = n_tp * part
    rows = 2 * tokens
    near = n_x * part

    fs = lax.axis_index("fs")
    tp = lax.axis_index("tp")
    z, y = lax.div(fs, n_y), lax.rem(fs, n_y)
    x, core = lax.div(tp, CORES), lax.rem(tp, CORES)
    mine = 1 - lax.rem(lax.rem(z, 2) + core, 2)

    def at_z(by):
        return {"fs": xor(z, by, n_z) * n_y + y}

    def at_y(by):
        return {"fs": z * n_y + xor(y, by, n_y)}

    def at_x(by):
        return {"tp": xor(x, by, n_x) * CORES + core}

    at_core = {"tp": x * CORES + 1 - core}

    def place(zr, yr):
        return xor(z, zr, n_z) * n_y + xor(y, yr, n_y)

    def first(where, tp_there=tp):
        quarter = lax.div(where, per_quarter)
        turned = 0
        k = 1
        while k < n_tp:
            turned = turned + k * lax.rem(lax.div(quarter, k) + lax.div(tp_there, k), 2)
            k *= 2
        slot = lax.rem(turned, CORES) * n_x + lax.div(turned, CORES)
        return slot * part + lax.rem(where, per_quarter) * depth

    def span(start, size):
        return pl.ds(pl.multiple_of(start, depth), size)

    def remote(src, dst, sems, index, device):
        return pltpu.make_async_remote_copy(
            src_ref=src,
            dst_ref=dst,
            send_sem=sems.at[(0, *index)],
            recv_sem=sems.at[(1, *index)],
            device_id=device,
            device_id_type=pl.DeviceIdType.MESH,
        )

    barrier = pltpu.get_barrier_semaphore()
    partners = (
        [at_core, at_z(1)]
        + [at_z(e) for e in far]
        + [at_y(d) for d in range(1, n_y)]
        + [at_x(d) for d in range(1, n_x)]
    )
    for partner in partners:
        pl.semaphore_signal(
            barrier, inc=1, device_id=partner, device_id_type=pl.DeviceIdType.MESH
        )

    shards = (gate_matrix, up_matrix, down_matrix)
    sources = (layer_input, out_cotangent)
    here = first(fs)
    kept_row = mine * here + (1 - mine) * model
    sent_row = mine * first(fs, x * CORES + 1 - core) + (1 - mine) * model

    def keep_shard(m):
        return pltpu.make_async_copy(
            shards[m].at[:, span(core * half, half)],
            w.at[m, span(kept_row, depth), :],
            local_sem.at[m],
        )

    def keep_tokens(k):
        return pltpu.make_async_copy(
            sources[k], xg.at[k, pl.ds(0, tokens), pl.ds(0, part)], local_sem.at[3 + k]
        )

    def swap_shard(m):
        return remote(
            shards[m].at[:, span((1 - core) * half, half)],
            w.at[m, span(sent_row, depth), :],
            ag_core,
            (m,),
            at_core,
        )

    def near_shard(m):
        return remote(
            w.at[m, pl.ds(model, depth), :], w.at[m, span(here, depth), :], ag_near, (m,), at_z(1)
        )

    def far_shard(m, e, s):
        block = w.at[m, span(first(place(s, 0)), depth), :]
        return remote(block, block, ag_far, (m, e - 2 + s), at_z(e))

    def y_shard(m, zr, yr):
        block = w.at[m, span(first(place(zr, 0)), depth), :]
        return remote(block, block, ag_y, (m, zr, yr - 1), at_y(yr))

    def token_z(k):
        return remote(
            sources[k], xg.at[k, pl.ds(tokens, tokens), pl.ds(0, part)], tok_z, (k,), at_z(1)
        )

    def token_x(k, p, xr):
        src = xg.at[k, pl.ds(tokens, tokens), pl.ds(0, part)] if p else sources[k]
        dst = xg.at[k, pl.ds(p * tokens, tokens), pl.ds(xr * part, part)]
        return remote(src, dst, tok_x, (k, p, xr - 1), at_x(xr))

    def token_core(k):
        return remote(
            xg.at[k, :, pl.ds(0, near)], xg.at[k, :, pl.ds(near, near)], tok_core, (k,), at_core
        )

    def send_y_shards(m, zr):
        for yr in range(1, n_y):
            y_shard(m, zr, yr).start()

    for m in range(3):
        keep_shard(m).start()
    for k in range(2):
        keep_tokens(k).start()
    pl.semaphore_wait(barrier, len(partners))

    for m in range(3):
        swap_shard(m).start()
    for k in range(2):
        for xr in range(1, n_x):
            token_x(k, 0, xr).start()
    for m in (GATE, UP):
        keep_shard(m).wait()
        swap_shard(m).wait_recv()
        near_shard(m).start()
        send_y_shards(m, 0)
    token_z(0).start()
    for m in (GATE, UP):
        for e in far:
            far_shard(m, e, 0).start()
    keep_shard(DOWN).wait()
    swap_shard(DOWN).wait_recv()
    send_y_shards(DOWN, 0)
    for m in (GATE, UP):
        near_shard(m).wait_recv()
        for e in far:
            far_shard(m, e, 1).start()
        send_y_shards(m, 1)
    token_z(1).start()
    near_shard(DOWN).start()
    token_z(0).wait_recv()
    for xr in range(1, n_x):
        token_x(0, 1, xr).start()
    for m in (GATE, UP):
        for e in far:
            far_shard(m, e, 0).wait_recv()
            send_y_shards(m, e)
    for e in far:
        far_shard(DOWN, e, 0).start()
    keep_tokens(0).wait()
    for p in range(2):
        for xr in range(1, n_x):
            token_x(0, p, xr).wait_recv()
    token_core(0).start()
    for m in (GATE, UP):
        for e in far:
            far_shard(m, e, 1).wait_recv()
            send_y_shards(m, e + 1)

    def arrived(m):
        for zr in range(n_z):
            for yr in range(1, n_y):
                y_shard(m, zr, yr).wait_recv()

    arrived(GATE)
    arrived(UP)
    token_core(0).wait_recv()

    def tile_of(i):
        return pl.ds(pl.multiple_of(i * TILE, TILE), TILE)

    strips = [slice(s * half // STRIPS, (s + 1) * half // STRIPS) for s in range(STRIPS)]

    def first_stage(begin, end):
        @pl.loop(begin, end)
        def _(i):
            tile = tile_of(i)
            mine_rows = xg[0, tile, :]
            for cols in strips:
                gate_pre = dot(mine_rows, w[GATE, :model, cols], NN)
                up_pre = dot(mine_rows, w[UP, :model, cols], NN)
                sigmoid_gate = jax.nn.sigmoid(gate_pre)
                activation = gate_pre * sigmoid_gate
                ab[0, tile, cols] = activation
                ab[1, tile, cols] = up_pre * sigmoid_gate * (1.0 + gate_pre * (1.0 - sigmoid_gate))
                delta[DOWN, tile, cols] = narrow(activation * up_pre)

    tiles = rows // TILE
    first_stage(0, tiles // 3)
    token_z(1).wait_recv()
    for xr in range(1, n_x):
        token_x(1, 1, xr).start()
    first_stage(tiles // 3, 2 * tiles // 3)
    near_shard(DOWN).wait_recv()
    for e in far:
        far_shard(DOWN, e, 1).start()
    send_y_shards(DOWN, 1)
    first_stage(2 * tiles // 3, tiles)
    keep_tokens(1).wait()
    for p in range(2):
        for xr in range(1, n_x):
            token_x(1, p, xr).wait_recv()
    token_core(1).start()
    for e in far:
        far_shard(DOWN, e, 0).wait_recv()
        send_y_shards(DOWN, e)
    token_core(1).wait_recv()

    def term(m, zr, yr):
        cols = span(first(place(zr, yr)), depth)
        pieces = [pl.ds(p * tokens, tokens) for p in range(2)]
        return sum(dot(xg[lax.div(m, 2), piece, cols], delta[m, piece, :], TN) for piece in pieces)

    def y_term(m, zr, yr):
        return remote(
            y_out.at[m, zr, yr - 1], y_in.at[m, zr, yr - 1], rs_y, (m, zr, yr - 1), at_y(yr)
        )

    def far_sum(m, zr, e):
        return remote(y_out.at[m, zr, 0], far_in.at[m, zr - 2], rs_far, (m, zr - 2), at_z(e))

    def near_sum(m):
        return remote(y_out.at[m, 1, 0], near_in.at[m], rs_near, (m,), at_z(1))

    def core_sum(m):
        return remote(y_out.at[m, 0, 0], core_in.at[m], rs_core, (m,), at_core)

    def send_y(m, zr):
        for yr in range(1, n_y):
            y_out[m, zr, yr - 1] = narrow(term(m, zr, yr))
            y_term(m, zr, yr).start()

    def y_sum(m, zr):
        total = term(m, zr, 0)
        for yr in range(1, n_y):
            y_term(m, zr, yr).wait_recv()
            total = total + wide(y_in[m, zr, yr - 1])
        y_term(m, zr, 1).wait_send()
        return total

    def cross(m, zr, e):
        y_out[m, zr, 0] = narrow(y_sum(m, zr))
        far_sum(m, zr, e).start()

    def pair(m):
        total = y_sum(m, 1)
        for e in far:
            far_sum(m, e + 1, e).wait_recv()
            total = total + wide(far_in[m, e - 1])
        y_out[m, 1, 0] = narrow(total)
        near_sum(m).start()

    def own_stage(m):
        return pl.ds(pl.multiple_of((2 * m + core) * depth, depth), depth)

    def other_stage(m):
        return pl.ds(pl.multiple_of((2 * m + 1 - core) * depth, depth), depth)

    def own(m):
        total = y_sum(m, 0)
        for e in far:
            far_sum(m, e, e).wait_recv()
            total = total + wide(far_in[m, e - 2])
        near_sum(m).wait_recv()
        other = wide(near_in[m])
        y_out[m, 0, 0] = narrow(jnp.where(mine == 1, other, total))
        core_sum(m).start()
        ab[0, own_stage(m), :] = jnp.where(mine == 1, total, other)

    def put(m):
        out = (gate_grad, up_grad, down_grad)[m]
        return [
            pltpu.make_async_copy(
                ab.at[0, pl.ds((2 * m + p) * depth, depth), :],
                out.at[:, pl.ds(p * half, half)],
                out_sem.at[m, p],
            )
            for p in range(2)
        ]

    def finish(m):
        core_sum(m).wait_recv()
        ab[0, other_stage(m), :] = wide(core_in[m])
        for copy in put(m):
            copy.start()

    @pl.loop(0, n_z - 2)
    def _(i):
        send_y(DOWN, n_z - 1 - i)

    for e in far:
        far_shard(DOWN, e, 1).wait_recv()
        send_y_shards(DOWN, e + 1)
    arrived(DOWN)

    def second_stage(begin, end):
        @pl.loop(begin, end)
        def _(i):
            tile = tile_of(i)
            mine_rows = xg[1, tile, :]
            for cols in strips:
                hidden_delta = dot(mine_rows, w[DOWN, :model, cols], NN)
                delta[UP, tile, cols] = narrow(hidden_delta * ab[0, tile, cols])
                delta[GATE, tile, cols] = narrow(hidden_delta * ab[1, tile, cols])

    second_stage(0, tiles)

    @pl.loop(0, 2 * (n_z - 2))
    def _(i):
        send_y(lax.rem(i, 2), n_z - 1 - lax.div(i, 2))

    for e in far:
        for s in (1, 0):
            cross(DOWN, e + s, e)

    @pl.loop(0, 2)
    def _(i):
        send_y(DOWN, 1 - i)

    @pl.loop(0, 4)
    def _(i):
        send_y(lax.rem(i, 2), 1 - lax.div(i, 2))

    for e in far:

        @pl.loop(0, 2)
        def _(m):
            cross(m, e + 1, e)

    def dx_tile(tile, begin):
        total = dot(delta[GATE, tile, :], w[GATE, begin : begin + part, :], NT)
        return total + dot(delta[UP, tile, :], w[UP, begin : begin + part, :], NT)

    dx_swap = remote(dx_out, dx_core, dx_core_sem, (), at_core)

    @pl.loop(0, tiles)
    def _(i):
        tile = tile_of(i)
        for xr in range(n_x):
            cols = pl.ds(xr * part, part)
            dx_out[tile, cols] = narrow(dx_tile(tile, near + xr * part))

    dx_swap.start()

    for e in far:

        @pl.loop(0, 2)
        def _(m):
            cross(m, e, e)

    dx_swap.wait_recv()

    @pl.loop(0, tiles)
    def _(i):
        tile = tile_of(i)
        for xr in range(n_x):
            cols = pl.ds(xr * part, part)
            dx_core[tile, cols] = narrow(dx_tile(tile, xr * part) + wide(dx_core[tile, cols]))

    def dx_over_x(xr):
        return remote(
            dx_core.at[:, pl.ds(xr * part, part)], dx_x.at[xr - 1], dx_x_sem, (xr - 1,), at_x(xr)
        )

    for xr in range(1, n_x):
        dx_over_x(xr).start()

    pair(DOWN)
    own(DOWN)
    finish(DOWN)

    for xr in range(1, n_x):
        dx_over_x(xr).wait_recv()

    @pl.loop(0, tiles)
    def _(i):
        tile = tile_of(i)
        total = wide(dx_core[tile, pl.ds(0, part)])
        for xr in range(1, n_x):
            total = total + wide(dx_x[xr - 1, tile, :])
        dx_core[tile, pl.ds(0, part)] = narrow(total)

    dx_over_z = remote(
        dx_core.at[pl.ds(tokens, tokens), pl.ds(0, part)], dx_z, dx_z_sem, (), at_z(1)
    )
    dx_over_z.start()

    @pl.loop(0, 2)
    def _(m):
        pair(m)

    dx_over_z.wait_recv()

    @pl.loop(0, tokens // TILE)
    def _(i):
        tile = tile_of(i)
        dx_z[tile, :] = narrow(wide(dx_core[tile, pl.ds(0, part)]) + wide(dx_z[tile, :]))

    put_dx = pltpu.make_async_copy(dx_z, input_grad, local_sem.at[5])
    put_dx.start()

    @pl.loop(0, 2)
    def _(m):
        own(m)

    for m in (GATE, UP):
        finish(m)

    dx_swap.wait_send()
    dx_over_z.wait_send()
    for xr in range(1, n_x):
        dx_over_x(xr).wait_send()
    for k in range(2):
        token_z(k).wait_send()
        token_core(k).wait_send()
        for p in range(2):
            for xr in range(1, n_x):
                token_x(k, p, xr).wait_send()
    for m in range(3):
        swap_shard(m).wait_send()
        near_shard(m).wait_send()
        near_sum(m).wait_send()
        core_sum(m).wait_send()
        for e in far:
            for s in range(2):
                far_shard(m, e, s).wait_send()
                far_sum(m, e + s, e).wait_send()
        for zr in range(n_z):
            for yr in range(1, n_y):
                y_shard(m, zr, yr).wait_send()
                if yr > 1:
                    y_term(m, zr, yr).wait_send()
        for copy in put(m):
            copy.wait()
    put_dx.wait()


def make(n_fs, n_tp):
    n_x = n_tp // CORES
    n_y = n_x
    n_z = n_fs // n_y

    def on_device(layer_input, out_cotangent, gate_matrix, up_matrix, down_matrix):
        tokens, part = layer_input.shape
        depth, width = gate_matrix.shape
        half = width // 2
        model = n_tp * part
        rows = 2 * tokens
        near = n_x * part
        bf16, f32 = jnp.bfloat16, jnp.float32
        sem = pltpu.SemaphoreType.DMA
        any_space = pl.BlockSpec(memory_space=pl.ANY)
        wide_grad = jax.ShapeDtypeStruct((depth, width), f32)
        flops = 2 * 8 * rows * half * model
        input_grad, gate_grad, up_grad, down_grad = pl.pallas_call(
            functools.partial(kernel, n_fs, n_tp),
            out_shape=(
                jax.ShapeDtypeStruct((tokens, part), bf16),
                wide_grad,
                wide_grad,
                wide_grad,
            ),
            in_specs=[any_space] * 5,
            out_specs=(any_space,) * 4,
            scratch_shapes=[
                pltpu.VMEM((2, rows, model), bf16),
                pltpu.VMEM((3, model + depth, half), bf16),
                pltpu.VMEM((2, rows, half), f32),
                pltpu.VMEM((3, rows, half), bf16),
                pltpu.VMEM((3, n_z, n_y - 1, depth, half), bf16),
                pltpu.VMEM((3, n_z, n_y - 1, depth, half), bf16),
                pltpu.VMEM((3, n_z - 2, depth, half), bf16),
                pltpu.VMEM((3, depth, half), bf16),
                pltpu.VMEM((3, depth, half), bf16),
                pltpu.VMEM((rows, near), bf16),
                pltpu.VMEM((rows, near), bf16),
                pltpu.VMEM((n_x - 1, rows, part), bf16),
                pltpu.VMEM((tokens, part), bf16),
                sem((6,)),
                sem((3, 2)),
                sem((2, 3)),
                sem((2, 3)),
                sem((2, 3, n_z - 2)),
                sem((2, 3, n_z, n_y - 1)),
                sem((2, 2)),
                sem((2, 2, 2, n_x - 1)),
                sem((2, 2)),
                sem((2, 3, n_z, n_y - 1)),
                sem((2, 3, n_z - 2)),
                sem((2, 3)),
                sem((2, 3)),
                sem((2,)),
                sem((2, n_x - 1)),
                sem((2,)),
            ],
            compiler_params=pltpu.CompilerParams(
                collective_id=0, has_side_effects=True, vmem_limit_bytes=67043328
            ),
            cost_estimate=pl.CostEstimate(
                flops=flops, bytes_accessed=rows * model, transcendentals=rows * half
            ),
        )(layer_input, out_cotangent, gate_matrix, up_matrix, down_matrix.T)
        return input_grad, gate_grad, up_grad, down_grad.T

    return on_device


def solution(mesh):
    return jax.shard_map(
        make(mesh.shape["fs"], mesh.shape["tp"]),
        mesh=mesh,
        in_specs=(P("fs", "tp"), P("fs", "tp"), P("fs", "tp"), P("fs", "tp"), P("tp", "fs")),
        out_specs=(P("fs", "tp"), P("fs", "tp"), P("fs", "tp"), P("tp", "fs")),
        check_vma=False,
    )
```

```python
import functools

import jax
import jax.numpy as jnp
from jax import lax
from jax.experimental import pallas as pl
from jax.experimental.pallas import tpu as pltpu
from jax.sharding import PartitionSpec as P

CORES = 2
TILE = 256
STRIPS = 3
HALVES = 2
PIECES = 3

NN = ((1,), (0,))
TN = ((0,), (0,))
NT = ((1,), (1,))

GATE, UP, DOWN = range(3)


def dot(left, right, dims):
    return lax.dot_general(left, right, (dims, ((), ())), preferred_element_type=jnp.float32)


def narrow(value):
    return value.astype(jnp.bfloat16)


def wide(value):
    return value.astype(jnp.float32)


def xor(left, right, n):
    total = 0
    k = 1
    while k < n:
        total = total + k * lax.rem(lax.div(left, k) + right // k % 2, 2)
        k *= 2
    return total


def kernel(
    n_fs,
    n_tp,
    layer_input,
    out_cotangent,
    gate_matrix,
    up_matrix,
    down_matrix,
    input_grad,
    gate_grad,
    up_grad,
    down_grad,
    xg,
    w,
    ab,
    delta,
    y_out,
    y_in,
    far_in,
    near_in,
    core_in,
    dx_out,
    dx_core,
    dx_x,
    dx_z,
    local_sem,
    out_sem,
    ag_core,
    ag_near,
    ag_far,
    ag_y,
    tok_z,
    tok_x,
    tok_core,
    rs_y,
    rs_far,
    rs_near,
    rs_core,
    dx_core_sem,
    dx_x_sem,
    dx_z_sem,
):
    n_x = n_tp // CORES
    n_y = n_x
    n_z = n_fs // n_y
    per_quarter = n_fs // n_tp
    far = range(2, n_z, 2)
    tokens, part = layer_input.shape
    depth, width = gate_matrix.shape
    half = width // 2
    model = n_tp * part
    rows = 2 * tokens
    near = n_x * part

    fs = lax.axis_index("fs")
    tp = lax.axis_index("tp")
    z, y = lax.div(fs, n_y), lax.rem(fs, n_y)
    x, core = lax.div(tp, CORES), lax.rem(tp, CORES)
    mine = 1 - lax.rem(lax.rem(z, 2) + core, 2)

    def at_z(by):
        return {"fs": xor(z, by, n_z) * n_y + y}

    def at_y(by):
        return {"fs": z * n_y + xor(y, by, n_y)}

    def at_x(by):
        return {"tp": xor(x, by, n_x) * CORES + core}

    at_core = {"tp": x * CORES + 1 - core}

    def place(zr, yr):
        return xor(z, zr, n_z) * n_y + xor(y, yr, n_y)

    def first(where, tp_there=tp):
        quarter = lax.div(where, per_quarter)
        turned = 0
        k = 1
        while k < n_tp:
            turned = turned + k * lax.rem(lax.div(quarter, k) + lax.div(tp_there, k), 2)
            k *= 2
        slot = lax.rem(turned, CORES) * n_x + lax.div(turned, CORES)
        return slot * part + lax.rem(where, per_quarter) * depth

    def span(start, size):
        return pl.ds(pl.multiple_of(start, depth), size)

    def remote(src, dst, sems, index, device):
        return pltpu.make_async_remote_copy(
            src_ref=src,
            dst_ref=dst,
            send_sem=sems.at[(0, *index)],
            recv_sem=sems.at[(1, *index)],
            device_id=device,
            device_id_type=pl.DeviceIdType.MESH,
        )

    barrier = pltpu.get_barrier_semaphore()
    partners = (
        [at_core, at_z(1)]
        + [at_z(e) for e in far]
        + [at_y(d) for d in range(1, n_y)]
        + [at_x(d) for d in range(1, n_x)]
    )
    for partner in partners:
        pl.semaphore_signal(
            barrier, inc=1, device_id=partner, device_id_type=pl.DeviceIdType.MESH
        )

    shards = (gate_matrix, up_matrix)
    sources = (layer_input, out_cotangent)
    here = first(fs)
    kept_row = mine * here + (1 - mine) * model
    sent_row = mine * first(fs, x * CORES + 1 - core) + (1 - mine) * model

    def load_down():
        return pltpu.make_async_copy(
            down_matrix, dx_core.at[pl.ds(0, width), pl.ds(0, depth)], local_sem.at[DOWN]
        )

    def turn_down():
        load_down().wait()
        w[DOWN, span(kept_row, depth), :] = dx_core[span(core * half, half), :depth].T
        y_out[DOWN, 0, 0] = dx_core[span((1 - core) * half, half), :depth].T

    def keep_shard(m):
        return pltpu.make_async_copy(
            shards[m].at[:, span(core * half, half)],
            w.at[m, span(kept_row, depth), :],
            local_sem.at[m],
        )

    def keep_tokens(k):
        return pltpu.make_async_copy(
            sources[k], xg.at[k, pl.ds(0, tokens), pl.ds(0, part)], local_sem.at[3 + k]
        )

    def swap_shard(m):
        if m == DOWN:
            src = y_out.at[DOWN, 0, 0]
        else:
            src = shards[m].at[:, span((1 - core) * half, half)]
        return remote(
            src,
            w.at[m, span(sent_row, depth), :],
            ag_core,
            (m,),
            at_core,
        )

    def near_shard(m):
        return remote(
            w.at[m, pl.ds(model, depth), :], w.at[m, span(here, depth), :], ag_near, (m,), at_z(1)
        )

    def far_shard(m, e, s):
        block = w.at[m, span(first(place(s, 0)), depth), :]
        return remote(block, block, ag_far, (m, e - 2 + s), at_z(e))

    def y_shard(m, zr, yr):
        block = w.at[m, span(first(place(zr, 0)), depth), :]
        return remote(block, block, ag_y, (m, zr, yr - 1), at_y(yr))

    piece = tokens // PIECES

    def token_z(k, h):
        return remote(
            sources[k].at[pl.ds(h * piece, piece), :],
            xg.at[k, pl.ds(tokens + h * piece, piece), pl.ds(0, part)],
            tok_z,
            (k, h),
            at_z(1),
        )

    def token_x(k, p, xr):
        here = pl.ds(tokens + (p - 1) * piece, piece) if p else pl.ds(0, tokens)
        src = xg.at[k, here, pl.ds(0, part)] if p else sources[k]
        dst = xg.at[k, here, pl.ds(xr * part, part)]
        return remote(src, dst, tok_x, (k, p, xr - 1), at_x(xr))

    def token_core(k, p):
        here = pl.ds(tokens + (p - 1) * piece, piece) if p else pl.ds(0, tokens)
        return remote(
            xg.at[k, here, pl.ds(0, near)],
            xg.at[k, here, pl.ds(near, near)],
            tok_core,
            (k, p),
            at_core,
        )

    def pass_tokens(k, h):
        token_z(k, h).wait_recv()
        for xr in range(1, n_x):
            token_x(k, 1 + h, xr).start()

    def join_tokens(k, p):
        if p == 0:
            keep_tokens(k).wait()
        for xr in range(1, n_x):
            token_x(k, p, xr).wait_recv()
        token_core(k, p).start()

    def await_tokens(k):
        for p in range(1 + PIECES):
            token_core(k, p).wait_recv()

    def relay_near(m):
        near_shard(m).wait_recv()
        for e in far:
            far_shard(m, e, 1).start()
        send_y_shards(m, 1)

    def relay_far(m, s):
        for e in far:
            far_shard(m, e, s).wait_recv()
            send_y_shards(m, e + s)

    def start_last():
        for h in range(PIECES):
            token_z(1, h).start()
        near_shard(DOWN).start()


    def send_y_shards(m, zr):
        for yr in range(1, n_y):
            y_shard(m, zr, yr).start()

    for m in (GATE, UP):
        keep_shard(m).start()
    load_down().start()
    for k in range(2):
        keep_tokens(k).start()
    pl.semaphore_wait(barrier, len(partners))

    for m in (GATE, UP):
        swap_shard(m).start()
    for k in range(2):
        for xr in range(1, n_x):
            token_x(k, 0, xr).start()
    for m in (GATE, UP):
        keep_shard(m).wait()
        swap_shard(m).wait_recv()
        near_shard(m).start()
        send_y_shards(m, 0)
    for h in range(PIECES):
        token_z(0, h).start()
    for m in (GATE, UP):
        for e in far:
            far_shard(m, e, 0).start()
    turn_down()
    swap_shard(DOWN).start()
    swap_shard(DOWN).wait_recv()
    send_y_shards(DOWN, 0)
    outer = lax.div(jnp.abs(2 * z - (n_z - 1)), n_z - 1)

    @pl.when(outer == 0)
    def _():
        for m in (GATE, UP):
            relay_near(m)
        start_last()
        for h in range(PIECES):
            pass_tokens(0, h)
        for m in (GATE, UP):
            relay_far(m, 0)
        for p in range(1 + PIECES):
            join_tokens(0, p)
        for m in (GATE, UP):
            relay_far(m, 1)

    @pl.when(outer == 1)
    def _():
        for m in (GATE, UP):
            relay_far(m, 0)
        for m in (GATE, UP):
            relay_near(m)
        for m in (GATE, UP):
            relay_far(m, 1)
        start_last()
        for h in range(PIECES):
            pass_tokens(0, h)
            join_tokens(0, h)
        join_tokens(0, PIECES)

    for e in far:
        far_shard(DOWN, e, 0).start()

    def arrived(m):
        for zr in range(n_z):
            for yr in range(1, n_y):
                y_shard(m, zr, yr).wait_recv()

    arrived(GATE)
    arrived(UP)
    await_tokens(0)

    def tile_of(i):
        return pl.ds(pl.multiple_of(i * TILE, TILE), TILE)

    strips = [slice(s * half // STRIPS, (s + 1) * half // STRIPS) for s in range(STRIPS)]

    def first_stage(begin, end):
        @pl.loop(begin, end)
        def _(i):
            tile = tile_of(i)
            mine_rows = xg[0, tile, :]
            for cols in strips:
                gate_pre = dot(mine_rows, w[GATE, :model, cols], NN)
                up_pre = dot(mine_rows, w[UP, :model, cols], NN)
                sigmoid_gate = jax.nn.sigmoid(gate_pre)
                activation = gate_pre * sigmoid_gate
                ab[0, tile, cols] = activation
                ab[1, tile, cols] = up_pre * sigmoid_gate * (1.0 + gate_pre * (1.0 - sigmoid_gate))
                delta[DOWN, tile, cols] = narrow(activation * up_pre)

    tiles = rows // TILE
    for h in range(PIECES):
        first_stage(h * tiles // PIECES, (h + 1) * tiles // PIECES)
        pass_tokens(1, h)
        join_tokens(1, h)
        if h == 0:

            @pl.when(outer == 1)
            def _():
                relay_far(DOWN, 0)

    relay_near(DOWN)
    join_tokens(1, PIECES)
    await_tokens(1)

    def term(m, zr, yr):
        cols = span(first(place(zr, yr)), depth)
        pieces = [pl.ds(p * tokens, tokens) for p in range(2)]
        return sum(dot(xg[lax.div(m, 2), piece, cols], delta[m, piece, :], TN) for piece in pieces)

    def y_term(m, zr, yr):
        return remote(
            y_out.at[m, zr, yr - 1], y_in.at[m, zr, yr - 1], rs_y, (m, zr, yr - 1), at_y(yr)
        )

    def far_sum(m, zr, e):
        return remote(y_out.at[m, zr, 0], far_in.at[m, zr - 2], rs_far, (m, zr - 2), at_z(e))

    def near_sum(m):
        return remote(y_out.at[m, 1, 0], near_in.at[m], rs_near, (m,), at_z(1))

    def core_sum(m):
        return remote(y_out.at[m, 0, 0], core_in.at[m], rs_core, (m,), at_core)

    def send_y(m, zr):
        for yr in range(1, n_y):
            y_out[m, zr, yr - 1] = narrow(term(m, zr, yr))
            y_term(m, zr, yr).start()

    def y_sum(m, zr):
        total = term(m, zr, 0)
        for yr in range(1, n_y):
            y_term(m, zr, yr).wait_recv()
            total = total + wide(y_in[m, zr, yr - 1])
        y_term(m, zr, 1).wait_send()
        return total

    def cross(m, zr, e):
        y_out[m, zr, 0] = narrow(y_sum(m, zr))
        far_sum(m, zr, e).start()

    def pair(m):
        total = y_sum(m, 1)
        for e in far:
            far_sum(m, e + 1, e).wait_recv()
            total = total + wide(far_in[m, e - 1])
        y_out[m, 1, 0] = narrow(total)
        near_sum(m).start()

    def own_stage(m):
        return pl.ds(pl.multiple_of((2 * m + core) * depth, depth), depth)

    def other_stage(m):
        return pl.ds(pl.multiple_of((2 * m + 1 - core) * depth, depth), depth)

    def own(m):
        total = y_sum(m, 0)
        for e in far:
            far_sum(m, e, e).wait_recv()
            total = total + wide(far_in[m, e - 2])
        near_sum(m).wait_recv()
        other = wide(near_in[m])
        y_out[m, 0, 0] = narrow(jnp.where(mine == 1, other, total))
        core_sum(m).start()
        kept = jnp.where(mine == 1, total, other)
        if m is DOWN:
            ab[1, span(core * half, half), :depth] = kept.T
        else:
            ab[0, own_stage(m), :] = kept

    def put(m):
        if m == DOWN:
            stage = ab.at[1, pl.ds(0, width), pl.ds(0, depth)]
            return [pltpu.make_async_copy(stage, down_grad, out_sem.at[DOWN, 0])]
        out = (gate_grad, up_grad)[m]
        return [
            pltpu.make_async_copy(
                ab.at[0, pl.ds((2 * m + p) * depth, depth), :],
                out.at[:, pl.ds(p * half, half)],
                out_sem.at[m, p],
            )
            for p in range(2)
        ]

    def finish(m):
        core_sum(m).wait_recv()
        if m == DOWN:
            ab[1, span((1 - core) * half, half), :depth] = wide(core_in[m]).T
        else:
            ab[0, other_stage(m), :] = wide(core_in[m])
        for copy in put(m):
            copy.start()

    send_y(DOWN, 3)

    @pl.when(outer == 0)
    def _():
        relay_far(DOWN, 0)
        relay_far(DOWN, 1)

    @pl.when(outer == 1)
    def _():
        cross(DOWN, 3, 2)
        relay_far(DOWN, 1)

    @pl.loop(0, 2)
    def _(i):
        send_y(DOWN, 2 - i)

    @pl.when(outer == 0)
    def _():
        cross(DOWN, 3, 2)

    arrived(DOWN)

    def second_stage(begin, end):
        @pl.loop(begin, end)
        def _(i):
            tile = tile_of(i)
            mine_rows = xg[1, tile, :]
            for cols in strips:
                hidden_delta = dot(mine_rows, w[DOWN, :model, cols], NN)
                delta[UP, tile, cols] = narrow(hidden_delta * ab[0, tile, cols])
                delta[GATE, tile, cols] = narrow(hidden_delta * ab[1, tile, cols])

    second_stage(0, tiles)

    def dx_tile(tile, begin):
        total = dot(delta[GATE, tile, :], w[GATE, begin : begin + part, :], NT)
        return total + dot(delta[UP, tile, :], w[UP, begin : begin + part, :], NT)

    def dx_rows(p):
        return pl.ds(p * tokens, tokens)

    def dx_swap(p):
        here = dx_rows(p)
        return remote(dx_out.at[here, :], dx_core.at[here, :], dx_core_sem, (p,), at_core)

    def dx_over_x(p, xr):
        here = dx_rows(p)
        return remote(
            dx_core.at[here, pl.ds(xr * part, part)],
            dx_x.at[xr - 1, here, :],
            dx_x_sem,
            (p, xr - 1),
            at_x(xr),
        )

    dx_over_z = remote(
        dx_core.at[pl.ds(tokens, tokens), pl.ds(0, part)], dx_z, dx_z_sem, (), at_z(1)
    )

    def dx_tiles(p):
        return pl.loop(p * tiles // 2, (p + 1) * tiles // 2)

    def dx_give(p):
        @dx_tiles(p)
        def _(i):
            tile = tile_of(i)
            for xr in range(n_x):
                cols = pl.ds(xr * part, part)
                dx_out[tile, cols] = narrow(dx_tile(tile, near + xr * part))

        dx_swap(p).start()

    def dx_take(p):
        dx_swap(p).wait_recv()

        @dx_tiles(p)
        def _(i):
            tile = tile_of(i)
            for xr in range(n_x):
                cols = pl.ds(xr * part, part)
                dx_core[tile, cols] = narrow(dx_tile(tile, xr * part) + wide(dx_core[tile, cols]))

        for xr in range(1, n_x):
            dx_over_x(p, xr).start()

    def dx_sum(p):
        for xr in range(1, n_x):
            dx_over_x(p, xr).wait_recv()

        @dx_tiles(p)
        def _(i):
            tile = tile_of(i)
            total = wide(dx_core[tile, pl.ds(0, part)])
            for xr in range(1, n_x):
                total = total + wide(dx_x[xr - 1, tile, :])
            dx_core[tile, pl.ds(0, part)] = narrow(total)

    def send_pair(zr):
        @pl.loop(0, 2)
        def _(m):
            send_y(m, zr)

    dx_give(1)
    send_pair(3)
    cross(DOWN, 2, 2)
    dx_take(1)
    pair(DOWN)
    send_y(GATE, 1)
    dx_give(0)
    cross(GATE, 3, 2)
    send_y(UP, 1)
    dx_take(0)
    cross(UP, 3, 2)
    send_pair(2)
    dx_sum(1)
    dx_over_z.start()
    pair(GATE)
    swap_shard(DOWN).wait_send()
    send_y(DOWN, 0)
    send_y(GATE, 0)
    pair(UP)
    send_y(UP, 0)

    @pl.loop(0, 2)
    def _(m):
        cross(m, 2, 2)

    dx_sum(0)
    dx_over_z.wait_recv()

    @pl.loop(0, tokens // TILE)
    def _(i):
        tile = tile_of(i)
        dx_z[tile, :] = narrow(wide(dx_core[tile, pl.ds(0, part)]) + wide(dx_z[tile, :]))

    put_dx = pltpu.make_async_copy(dx_z, input_grad, local_sem.at[5])
    put_dx.start()
    own(DOWN)
    finish(DOWN)

    @pl.loop(0, 2)
    def _(m):
        own(m)

    for m in (GATE, UP):
        finish(m)

    dx_over_z.wait_send()
    for p in range(2):
        dx_swap(p).wait_send()
        for xr in range(1, n_x):
            dx_over_x(p, xr).wait_send()
    for k in range(2):
        for h in range(PIECES):
            token_z(k, h).wait_send()
        for p in range(1 + PIECES):
            token_core(k, p).wait_send()
            for xr in range(1, n_x):
                token_x(k, p, xr).wait_send()
    for m in range(3):
        if m != DOWN:
            swap_shard(m).wait_send()
        near_shard(m).wait_send()
        near_sum(m).wait_send()
        core_sum(m).wait_send()
        for e in far:
            for s in range(2):
                far_shard(m, e, s).wait_send()
                far_sum(m, e + s, e).wait_send()
        for zr in range(n_z):
            for yr in range(1, n_y):
                y_shard(m, zr, yr).wait_send()
                if yr > 1:
                    y_term(m, zr, yr).wait_send()
        for copy in put(m):
            copy.wait()
    put_dx.wait()


def hand_over(*refs):
    count = (len(refs) - 2) // 3
    sources, results, stages = refs[:count], refs[count : 2 * count], refs[2 * count : 3 * count]
    came, went = refs[3 * count :]

    def piece(ref, p):
        size = ref.shape[0] // HALVES
        return ref.at[pl.ds(p * size, size), :]

    def load(i, p):
        return pltpu.make_async_copy(piece(sources[i], p), piece(stages[i], p), came.at[i, p])

    def store(i, p):
        return pltpu.make_async_copy(piece(stages[i], p), piece(results[i], p), went.at[i, p])

    order = [(i, p) for i in range(count) for p in range(HALVES)]
    for i, p in order:
        load(i, p).start()
    for i, p in order:
        load(i, p).wait()
        store(i, p).start()
    for i, p in order:
        store(i, p).wait()


def copied(results):
    shapes = tuple(jax.ShapeDtypeStruct(r.shape, r.dtype) for r in results)
    any_space = pl.BlockSpec(memory_space=pl.ANY)
    sems = pltpu.SemaphoreType.DMA((len(results), HALVES))
    return pl.pallas_call(
        hand_over,
        out_shape=shapes,
        in_specs=[any_space] * len(results),
        out_specs=(any_space,) * len(results),
        scratch_shapes=[pltpu.VMEM(r.shape, r.dtype) for r in results] + [sems, sems],
    )(*results)


def make(n_fs, n_tp):
    n_x = n_tp // CORES
    n_y = n_x
    n_z = n_fs // n_y

    def on_device(layer_input, out_cotangent, gate_matrix, up_matrix, down_matrix):
        tokens, part = layer_input.shape
        depth, width = gate_matrix.shape
        half = width // 2
        model = n_tp * part
        rows = 2 * tokens
        near = n_x * part
        bf16, f32 = jnp.bfloat16, jnp.float32
        sem = pltpu.SemaphoreType.DMA
        any_space = pl.BlockSpec(memory_space=pl.ANY)
        wide_grad = jax.ShapeDtypeStruct((depth, width), f32)
        flops = 2 * 8 * rows * half * model
        results = pl.pallas_call(
            functools.partial(kernel, n_fs, n_tp),
            out_shape=(
                jax.ShapeDtypeStruct((tokens, part), bf16),
                wide_grad,
                wide_grad,
                jax.ShapeDtypeStruct((width, depth), f32),
            ),
            in_specs=[any_space] * 5,
            out_specs=(any_space,) * 4,
            scratch_shapes=[
                pltpu.VMEM((2, rows, model), bf16),
                pltpu.VMEM((3, model + depth, half), bf16),
                pltpu.VMEM((2, rows, half), f32),
                pltpu.VMEM((3, rows, half), bf16),
                pltpu.VMEM((3, n_z, n_y - 1, depth, half), bf16),
                pltpu.VMEM((3, n_z, n_y - 1, depth, half), bf16),
                pltpu.VMEM((3, n_z - 2, depth, half), bf16),
                pltpu.VMEM((3, depth, half), bf16),
                pltpu.VMEM((3, depth, half), bf16),
                pltpu.VMEM((rows, near), bf16),
                pltpu.VMEM((rows, near), bf16),
                pltpu.VMEM((n_x - 1, rows, part), bf16),
                pltpu.VMEM((tokens, part), bf16),
                sem((6,)),
                sem((3, 2)),
                sem((2, 3)),
                sem((2, 3)),
                sem((2, 3, n_z - 2)),
                sem((2, 3, n_z, n_y - 1)),
                sem((2, 2, PIECES)),
                sem((2, 2, 1 + PIECES, n_x - 1)),
                sem((2, 2, 1 + PIECES)),
                sem((2, 3, n_z, n_y - 1)),
                sem((2, 3, n_z - 2)),
                sem((2, 3)),
                sem((2, 3)),
                sem((2, 2)),
                sem((2, 2, n_x - 1)),
                sem((2,)),
            ],
            compiler_params=pltpu.CompilerParams(
                collective_id=0, has_side_effects=True, vmem_limit_bytes=67043328
            ),
            cost_estimate=pl.CostEstimate(
                flops=flops, bytes_accessed=rows * model, transcendentals=rows * half
            ),
        )(layer_input, out_cotangent, gate_matrix, up_matrix, down_matrix)
        return copied(results)

    return on_device


def solution(mesh):
    return jax.shard_map(
        make(mesh.shape["fs"], mesh.shape["tp"]),
        mesh=mesh,
        in_specs=(P("fs", "tp"), P("fs", "tp"), P("fs", "tp"), P("fs", "tp"), P("tp", "fs")),
        out_specs=(P("fs", "tp"), P("fs", "tp"), P("fs", "tp"), P("tp", "fs")),
        check_vma=False,
    )
```

```python
import functools

import jax
import jax.numpy as jnp
from jax import lax
from jax.experimental import pallas as pl
from jax.experimental.pallas import tpu as pltpu
from jax.sharding import PartitionSpec as P

CORES = 2
TILE = 256
STRIPS = 3
HALVES = 2
PIECES = 3

NN = ((1,), (0,))
TN = ((0,), (0,))
NT = ((1,), (1,))

GATE, UP, DOWN = range(3)


def dot(left, right, dims):
    return lax.dot_general(left, right, (dims, ((), ())), preferred_element_type=jnp.float32)


def narrow(value):
    return value.astype(jnp.bfloat16)


def wide(value):
    return value.astype(jnp.float32)


def xor(left, right, n):
    total = 0
    k = 1
    while k < n:
        total = total + k * lax.rem(lax.div(left, k) + right // k % 2, 2)
        k *= 2
    return total


def kernel(
    n_fs,
    n_tp,
    layer_input,
    out_cotangent,
    gate_matrix,
    up_matrix,
    down_matrix,
    input_grad,
    gate_grad,
    up_grad,
    down_grad,
    xg,
    w,
    ab,
    delta,
    y_out,
    y_in,
    far_in,
    direct_in,
    near_in,
    core_in,
    dx_out,
    dx_core,
    dx_x,
    dx_z,
    local_sem,
    out_sem,
    ag_core,
    ag_near,
    ag_far,
    ag_direct,
    ag_y,
    tok_z,
    tok_x,
    tok_core,
    rs_y,
    rs_far,
    rs_direct,
    rs_near,
    rs_core,
    dx_core_sem,
    dx_x_sem,
    dx_z_sem,
):
    n_x = n_tp // CORES
    n_y = n_x
    n_z = n_fs // n_y
    per_quarter = n_fs // n_tp
    far = range(2, n_z, 2)
    tokens, part = layer_input.shape
    depth, width = gate_matrix.shape
    half = width // 2
    model = n_tp * part
    rows = 2 * tokens
    near = n_x * part

    fs = lax.axis_index("fs")
    tp = lax.axis_index("tp")
    z, y = lax.div(fs, n_y), lax.rem(fs, n_y)
    x, core = lax.div(tp, CORES), lax.rem(tp, CORES)
    mine = 1 - lax.rem(lax.rem(z, 2) + core, 2)

    def at_z(by):
        return {"fs": xor(z, by, n_z) * n_y + y}

    def at_y(by):
        return {"fs": z * n_y + xor(y, by, n_y)}

    def at_x(by):
        return {"tp": xor(x, by, n_x) * CORES + core}

    at_core = {"tp": x * CORES + 1 - core}

    def place(zr, yr):
        return xor(z, zr, n_z) * n_y + xor(y, yr, n_y)

    def first(where, tp_there=tp):
        quarter = lax.div(where, per_quarter)
        turned = 0
        k = 1
        while k < n_tp:
            turned = turned + k * lax.rem(lax.div(quarter, k) + lax.div(tp_there, k), 2)
            k *= 2
        slot = lax.rem(turned, CORES) * n_x + lax.div(turned, CORES)
        return slot * part + lax.rem(where, per_quarter) * depth

    def span(start, size):
        return pl.ds(pl.multiple_of(start, depth), size)

    def remote(src, dst, sems, index, device):
        return pltpu.make_async_remote_copy(
            src_ref=src,
            dst_ref=dst,
            send_sem=sems.at[(0, *index)],
            recv_sem=sems.at[(1, *index)],
            device_id=device,
            device_id_type=pl.DeviceIdType.MESH,
        )

    barrier = pltpu.get_barrier_semaphore()
    partners = (
        [at_core, at_z(1)]
        + [at_z(e) for e in far]
        + [at_z(3)]
        + [at_y(d) for d in range(1, n_y)]
        + [at_x(d) for d in range(1, n_x)]
    )
    for partner in partners:
        pl.semaphore_signal(
            barrier, inc=1, device_id=partner, device_id_type=pl.DeviceIdType.MESH
        )

    outer = lax.div(jnp.abs(2 * z - (n_z - 1)), n_z - 1)
    at_ends = pl.when(outer == 1)
    at_inner = pl.when(outer == 0)

    shards = (gate_matrix, up_matrix)
    sources = (layer_input, out_cotangent)
    here = first(fs)
    kept_row = mine * here + (1 - mine) * model
    sent_row = mine * first(fs, x * CORES + 1 - core) + (1 - mine) * model

    def load_down():
        return pltpu.make_async_copy(
            down_matrix, dx_core.at[pl.ds(0, width), pl.ds(0, depth)], local_sem.at[DOWN]
        )

    def turn_down():
        load_down().wait()
        w[DOWN, span(kept_row, depth), :] = dx_core[span(core * half, half), :depth].T
        y_out[DOWN, 0, 0] = dx_core[span((1 - core) * half, half), :depth].T

    def keep_shard(m):
        return pltpu.make_async_copy(
            shards[m].at[:, span(core * half, half)],
            w.at[m, span(kept_row, depth), :],
            local_sem.at[m],
        )

    def keep_tokens(k):
        return pltpu.make_async_copy(
            sources[k], xg.at[k, pl.ds(0, tokens), pl.ds(0, part)], local_sem.at[3 + k]
        )

    def swap_shard(m):
        if m == DOWN:
            src = y_out.at[DOWN, 0, 0]
        else:
            src = shards[m].at[:, span((1 - core) * half, half)]
        return remote(
            src,
            w.at[m, span(sent_row, depth), :],
            ag_core,
            (m,),
            at_core,
        )

    def near_shard(m):
        return remote(
            w.at[m, pl.ds(model, depth), :], w.at[m, span(here, depth), :], ag_near, (m,), at_z(1)
        )

    def direct_shard(m):
        return remote(
            w.at[m, pl.ds(model, depth), :], w.at[m, span(here, depth), :], ag_direct, (m,), at_z(3)
        )

    def far_shard(m, e, s):
        block = w.at[m, span(first(place(s, 0)), depth), :]
        return remote(block, block, ag_far, (m, e - 2 + s), at_z(e))

    def y_shard(m, zr, yr):
        block = w.at[m, span(first(place(zr, 0)), depth), :]
        return remote(block, block, ag_y, (m, zr, yr - 1), at_y(yr))

    piece = tokens // PIECES

    def token_z(k, h):
        return remote(
            sources[k].at[pl.ds(h * piece, piece), :],
            xg.at[k, pl.ds(tokens + h * piece, piece), pl.ds(0, part)],
            tok_z,
            (k, h),
            at_z(1),
        )

    def token_x(k, p, xr):
        here = pl.ds(tokens + (p - 1) * piece, piece) if p else pl.ds(0, tokens)
        src = xg.at[k, here, pl.ds(0, part)] if p else sources[k]
        dst = xg.at[k, here, pl.ds(xr * part, part)]
        return remote(src, dst, tok_x, (k, p, xr - 1), at_x(xr))

    def token_core(k, p):
        here = pl.ds(tokens + (p - 1) * piece, piece) if p else pl.ds(0, tokens)
        return remote(
            xg.at[k, here, pl.ds(0, near)],
            xg.at[k, here, pl.ds(near, near)],
            tok_core,
            (k, p),
            at_core,
        )

    def pass_tokens(k, h):
        token_z(k, h).wait_recv()
        for xr in range(1, n_x):
            token_x(k, 1 + h, xr).start()

    def join_tokens(k, p):
        if p == 0:
            keep_tokens(k).wait()
        for xr in range(1, n_x):
            token_x(k, p, xr).wait_recv()
        token_core(k, p).start()

    def await_tokens(k):
        for p in range(1 + PIECES):
            token_core(k, p).wait_recv()

    def relay_near(m):
        near_shard(m).wait_recv()

        @at_inner
        def _():
            far_shard(m, 2, 1).start()

        send_y_shards(m, 1)

    def relay_far(m):
        far_shard(m, 2, 0).wait_recv()
        send_y_shards(m, 2)

    def relay_last(m):
        @at_inner
        def _():
            direct_shard(m).wait_recv()

        @at_ends
        def _():
            far_shard(m, 2, 1).wait_recv()

        send_y_shards(m, 3)


    def send_y_shards(m, zr):
        for yr in range(1, n_y):
            y_shard(m, zr, yr).start()

    for m in (GATE, UP):
        keep_shard(m).start()
    load_down().start()
    for k in range(2):
        keep_tokens(k).start()
    pl.semaphore_wait(barrier, len(partners))

    for m in (GATE, UP):
        swap_shard(m).start()
    for k in range(2):
        for xr in range(1, n_x):
            token_x(k, 0, xr).start()
    for m in (GATE, UP):
        keep_shard(m).wait()
        swap_shard(m).wait_recv()
        near_shard(m).start()
        send_y_shards(m, 0)
    for h in range(PIECES):
        token_z(0, h).start()
    for m in (GATE, UP):
        far_shard(m, 2, 0).start()

    @at_ends
    def _():
        direct_in[...] = jnp.zeros_like(direct_in)
        far_in[:, 1] = jnp.zeros((3, depth, half), far_in.dtype)

    turn_down()
    swap_shard(DOWN).start()
    swap_shard(DOWN).wait_recv()
    send_y_shards(DOWN, 0)
    @at_inner
    def _():
        for m in (GATE, UP):
            relay_near(m)
        for m in (GATE, UP):
            direct_shard(m).start()
        for h in range(PIECES):
            token_z(1, h).start()
        near_shard(DOWN).start()
        for h in range(PIECES):
            pass_tokens(0, h)
        for m in (GATE, UP):
            relay_far(m)
        for p in range(1 + PIECES):
            join_tokens(0, p)
        far_shard(DOWN, 2, 0).start()
        for m in (GATE, UP):
            relay_last(m)
        relay_near(DOWN)
        direct_shard(DOWN).start()

    @at_ends
    def _():
        near_shard(DOWN).start()
        for h in range(PIECES):
            token_z(1, h).start()
        far_shard(DOWN, 2, 0).start()
        for m in (GATE, UP):
            relay_far(m)
        for m in (GATE, UP):
            relay_last(m)
        for m in (GATE, UP):
            relay_near(m)
        for h in range(PIECES):
            pass_tokens(0, h)
            join_tokens(0, h)
        join_tokens(0, PIECES)

    def arrived(m):
        for zr in range(n_z):
            for yr in range(1, n_y):
                y_shard(m, zr, yr).wait_recv()

    arrived(GATE)
    arrived(UP)
    await_tokens(0)

    def tile_of(i):
        return pl.ds(pl.multiple_of(i * TILE, TILE), TILE)

    strips = [slice(s * half // STRIPS, (s + 1) * half // STRIPS) for s in range(STRIPS)]

    def first_stage(begin, end):
        @pl.loop(begin, end)
        def _(i):
            tile = tile_of(i)
            mine_rows = xg[0, tile, :]
            for cols in strips:
                gate_pre = dot(mine_rows, w[GATE, :model, cols], NN)
                up_pre = dot(mine_rows, w[UP, :model, cols], NN)
                sigmoid_gate = jax.nn.sigmoid(gate_pre)
                activation = gate_pre * sigmoid_gate
                ab[0, tile, cols] = activation
                ab[1, tile, cols] = up_pre * sigmoid_gate * (1.0 + gate_pre * (1.0 - sigmoid_gate))
                delta[DOWN, tile, cols] = narrow(activation * up_pre)

    tiles = rows // TILE
    for h in range(PIECES):
        first_stage(h * tiles // PIECES, (h + 1) * tiles // PIECES)
        pass_tokens(1, h)
        join_tokens(1, h)
        if h == 0:
            relay_far(DOWN)
        elif h == 1:

            @at_ends
            def _():
                relay_last(DOWN)

    @at_ends
    def _():
        relay_near(DOWN)

    join_tokens(1, PIECES)

    @at_inner
    def _():
        relay_last(DOWN)

    await_tokens(1)

    def term(m, zr, yr):
        cols = span(first(place(zr, yr)), depth)
        pieces = [pl.ds(p * tokens, tokens) for p in range(2)]
        return sum(dot(xg[lax.div(m, 2), piece, cols], delta[m, piece, :], TN) for piece in pieces)

    def y_term(m, zr, yr):
        return remote(
            y_out.at[m, zr, yr - 1], y_in.at[m, zr, yr - 1], rs_y, (m, zr, yr - 1), at_y(yr)
        )

    def far_sum(m, zr, e):
        return remote(y_out.at[m, zr, 0], far_in.at[m, zr - 2], rs_far, (m, zr - 2), at_z(e))

    def direct_sum(m):
        return remote(y_out.at[m, 3, 0], direct_in.at[m], rs_direct, (m,), at_z(3))

    def near_sum(m):
        return remote(y_out.at[m, 1, 0], near_in.at[m], rs_near, (m,), at_z(1))

    def core_sum(m):
        return remote(y_out.at[m, 0, 0], core_in.at[m], rs_core, (m,), at_core)

    def send_y(m, zr):
        for yr in range(1, n_y):
            y_out[m, zr, yr - 1] = narrow(term(m, zr, yr))
            y_term(m, zr, yr).start()

    def y_sum(m, zr):
        total = term(m, zr, 0)
        for yr in range(1, n_y):
            y_term(m, zr, yr).wait_recv()
            total = total + wide(y_in[m, zr, yr - 1])
        y_term(m, zr, 1).wait_send()
        return total

    def cross(m, zr, e):
        y_out[m, zr, 0] = narrow(y_sum(m, zr))
        if zr != 3:
            far_sum(m, zr, e).start()
            return

        @at_inner
        def _():
            direct_sum(m).start()

        @at_ends
        def _():
            far_sum(m, 3, 2).start()

    def pair(m):
        total = y_sum(m, 1)

        @at_inner
        def _():
            far_sum(m, 3, 2).wait_recv()

        y_out[m, 1, 0] = narrow(total + wide(far_in[m, 1]))
        near_sum(m).start()

    def own_stage(m):
        return pl.ds(pl.multiple_of((2 * m + core) * depth, depth), depth)

    def other_stage(m):
        return pl.ds(pl.multiple_of((2 * m + 1 - core) * depth, depth), depth)

    def own(m):
        total = y_sum(m, 0)
        for e in far:
            far_sum(m, e, e).wait_recv()
            total = total + wide(far_in[m, e - 2])
        near_sum(m).wait_recv()

        @at_inner
        def _():
            direct_sum(m).wait_recv()

        other = wide(near_in[m]) + wide(direct_in[m])
        y_out[m, 0, 0] = narrow(jnp.where(mine == 1, other, total))
        core_sum(m).start()
        kept = jnp.where(mine == 1, total, other)
        if m is DOWN:
            ab[1, span(core * half, half), :depth] = kept.T
        else:
            ab[0, own_stage(m), :] = kept

    def put(m):
        if m == DOWN:
            stage = ab.at[1, pl.ds(0, width), pl.ds(0, depth)]
            return [pltpu.make_async_copy(stage, down_grad, out_sem.at[DOWN, 0])]
        out = (gate_grad, up_grad)[m]
        return [
            pltpu.make_async_copy(
                ab.at[0, pl.ds((2 * m + p) * depth, depth), :],
                out.at[:, pl.ds(p * half, half)],
                out_sem.at[m, p],
            )
            for p in range(2)
        ]

    def finish(m):
        core_sum(m).wait_recv()
        if m == DOWN:
            ab[1, span((1 - core) * half, half), :depth] = wide(core_in[m]).T
        else:
            ab[0, other_stage(m), :] = wide(core_in[m])
        for copy in put(m):
            copy.start()

    @pl.loop(0, 3)
    def _(i):
        send_y(DOWN, 3 - i)

    arrived(DOWN)

    def second_stage(begin, end):
        @pl.loop(begin, end)
        def _(i):
            tile = tile_of(i)
            mine_rows = xg[1, tile, :]
            for cols in strips:
                hidden_delta = dot(mine_rows, w[DOWN, :model, cols], NN)
                delta[UP, tile, cols] = narrow(hidden_delta * ab[0, tile, cols])
                delta[GATE, tile, cols] = narrow(hidden_delta * ab[1, tile, cols])

    second_stage(0, tiles)

    def dx_tile(tile, begin):
        total = dot(delta[GATE, tile, :], w[GATE, begin : begin + part, :], NT)
        return total + dot(delta[UP, tile, :], w[UP, begin : begin + part, :], NT)

    def dx_rows(p):
        return pl.ds(p * tokens, tokens)

    def dx_swap(p):
        here = dx_rows(p)
        return remote(dx_out.at[here, :], dx_core.at[here, :], dx_core_sem, (p,), at_core)

    def dx_over_x(p, xr):
        here = dx_rows(p)
        return remote(
            dx_core.at[here, pl.ds(xr * part, part)],
            dx_x.at[xr - 1, here, :],
            dx_x_sem,
            (p, xr - 1),
            at_x(xr),
        )

    dx_over_z = remote(
        dx_core.at[pl.ds(tokens, tokens), pl.ds(0, part)], dx_z, dx_z_sem, (), at_z(1)
    )

    def dx_tiles(p):
        return pl.loop(p * tiles // 2, (p + 1) * tiles // 2)

    def dx_give(p):
        @dx_tiles(p)
        def _(i):
            tile = tile_of(i)
            for xr in range(n_x):
                cols = pl.ds(xr * part, part)
                dx_out[tile, cols] = narrow(dx_tile(tile, near + xr * part))

        dx_swap(p).start()

    def dx_take(p):
        dx_swap(p).wait_recv()

        @dx_tiles(p)
        def _(i):
            tile = tile_of(i)
            for xr in range(n_x):
                cols = pl.ds(xr * part, part)
                dx_core[tile, cols] = narrow(dx_tile(tile, xr * part) + wide(dx_core[tile, cols]))

        for xr in range(1, n_x):
            dx_over_x(p, xr).start()

    def dx_sum(p):
        for xr in range(1, n_x):
            dx_over_x(p, xr).wait_recv()

        @dx_tiles(p)
        def _(i):
            tile = tile_of(i)
            total = wide(dx_core[tile, pl.ds(0, part)])
            for xr in range(1, n_x):
                total = total + wide(dx_x[xr - 1, tile, :])
            dx_core[tile, pl.ds(0, part)] = narrow(total)

    def send_pair(zr):
        @pl.loop(0, 2)
        def _(m):
            send_y(m, zr)

    dx_give(1)
    cross(DOWN, 3, 2)
    send_pair(3)
    cross(DOWN, 2, 2)
    dx_take(1)
    pair(DOWN)
    send_y(GATE, 1)
    dx_give(0)
    cross(GATE, 3, 2)
    send_y(UP, 1)
    dx_take(0)
    cross(UP, 3, 2)
    send_pair(2)
    dx_sum(1)
    dx_over_z.start()
    pair(GATE)
    swap_shard(DOWN).wait_send()
    send_y(DOWN, 0)
    send_y(GATE, 0)
    pair(UP)
    send_y(UP, 0)

    @pl.loop(0, 2)
    def _(m):
        cross(m, 2, 2)

    dx_sum(0)
    dx_over_z.wait_recv()

    @pl.loop(0, tokens // TILE)
    def _(i):
        tile = tile_of(i)
        dx_z[tile, :] = narrow(wide(dx_core[tile, pl.ds(0, part)]) + wide(dx_z[tile, :]))

    put_dx = pltpu.make_async_copy(dx_z, input_grad, local_sem.at[5])
    put_dx.start()
    own(DOWN)
    finish(DOWN)

    @pl.loop(0, 2)
    def _(m):
        own(m)

    for m in (GATE, UP):
        finish(m)

    dx_over_z.wait_send()
    for p in range(2):
        dx_swap(p).wait_send()
        for xr in range(1, n_x):
            dx_over_x(p, xr).wait_send()
    for k in range(2):
        for h in range(PIECES):
            token_z(k, h).wait_send()
        for p in range(1 + PIECES):
            token_core(k, p).wait_send()
            for xr in range(1, n_x):
                token_x(k, p, xr).wait_send()
    for m in range(3):
        if m != DOWN:
            swap_shard(m).wait_send()
        near_shard(m).wait_send()
        near_sum(m).wait_send()
        core_sum(m).wait_send()
        far_shard(m, 2, 0).wait_send()
        far_sum(m, 2, 2).wait_send()

        @at_inner
        def _():
            far_shard(m, 2, 1).wait_send()
            direct_shard(m).wait_send()
            direct_sum(m).wait_send()

        @at_ends
        def _():
            far_sum(m, 3, 2).wait_send()

        for zr in range(n_z):
            for yr in range(1, n_y):
                y_shard(m, zr, yr).wait_send()
                if yr > 1:
                    y_term(m, zr, yr).wait_send()
        for copy in put(m):
            copy.wait()
    put_dx.wait()


def hand_over(*refs):
    count = (len(refs) - 2) // 3
    sources, results, stages = refs[:count], refs[count : 2 * count], refs[2 * count : 3 * count]
    came, went = refs[3 * count :]

    def piece(ref, p):
        size = ref.shape[0] // HALVES
        return ref.at[pl.ds(p * size, size), :]

    def load(i, p):
        return pltpu.make_async_copy(piece(sources[i], p), piece(stages[i], p), came.at[i, p])

    def store(i, p):
        return pltpu.make_async_copy(piece(stages[i], p), piece(results[i], p), went.at[i, p])

    order = [(i, p) for i in range(count) for p in range(HALVES)]
    for i, p in order:
        load(i, p).start()
    for i, p in order:
        load(i, p).wait()
        store(i, p).start()
    for i, p in order:
        store(i, p).wait()


def copied(results):
    shapes = tuple(jax.ShapeDtypeStruct(r.shape, r.dtype) for r in results)
    any_space = pl.BlockSpec(memory_space=pl.ANY)
    sems = pltpu.SemaphoreType.DMA((len(results), HALVES))
    return pl.pallas_call(
        hand_over,
        out_shape=shapes,
        in_specs=[any_space] * len(results),
        out_specs=(any_space,) * len(results),
        scratch_shapes=[pltpu.VMEM(r.shape, r.dtype) for r in results] + [sems, sems],
    )(*results)


def make(n_fs, n_tp):
    n_x = n_tp // CORES
    n_y = n_x
    n_z = n_fs // n_y

    def on_device(layer_input, out_cotangent, gate_matrix, up_matrix, down_matrix):
        tokens, part = layer_input.shape
        depth, width = gate_matrix.shape
        half = width // 2
        model = n_tp * part
        rows = 2 * tokens
        near = n_x * part
        bf16, f32 = jnp.bfloat16, jnp.float32
        sem = pltpu.SemaphoreType.DMA
        any_space = pl.BlockSpec(memory_space=pl.ANY)
        wide_grad = jax.ShapeDtypeStruct((depth, width), f32)
        flops = 2 * 8 * rows * half * model
        results = pl.pallas_call(
            functools.partial(kernel, n_fs, n_tp),
            out_shape=(
                jax.ShapeDtypeStruct((tokens, part), bf16),
                wide_grad,
                wide_grad,
                jax.ShapeDtypeStruct((width, depth), f32),
            ),
            in_specs=[any_space] * 5,
            out_specs=(any_space,) * 4,
            scratch_shapes=[
                pltpu.VMEM((2, rows, model), bf16),
                pltpu.VMEM((3, model + depth, half), bf16),
                pltpu.VMEM((2, rows, half), f32),
                pltpu.VMEM((3, rows, half), bf16),
                pltpu.VMEM((3, n_z, n_y - 1, depth, half), bf16),
                pltpu.VMEM((3, n_z, n_y - 1, depth, half), bf16),
                pltpu.VMEM((3, n_z - 2, depth, half), bf16),
                pltpu.VMEM((3, depth, half), bf16),
                pltpu.VMEM((3, depth, half), bf16),
                pltpu.VMEM((3, depth, half), bf16),
                pltpu.VMEM((rows, near), bf16),
                pltpu.VMEM((rows, near), bf16),
                pltpu.VMEM((n_x - 1, rows, part), bf16),
                pltpu.VMEM((tokens, part), bf16),
                sem((6,)),
                sem((3, 2)),
                sem((2, 3)),
                sem((2, 3)),
                sem((2, 3, n_z - 2)),
                sem((2, 3)),
                sem((2, 3, n_z, n_y - 1)),
                sem((2, 2, PIECES)),
                sem((2, 2, 1 + PIECES, n_x - 1)),
                sem((2, 2, 1 + PIECES)),
                sem((2, 3, n_z, n_y - 1)),
                sem((2, 3, n_z - 2)),
                sem((2, 3)),
                sem((2, 3)),
                sem((2, 3)),
                sem((2, 2)),
                sem((2, 2, n_x - 1)),
                sem((2,)),
            ],
            compiler_params=pltpu.CompilerParams(
                collective_id=0, has_side_effects=True, vmem_limit_bytes=67043328
            ),
            cost_estimate=pl.CostEstimate(
                flops=flops, bytes_accessed=rows * model, transcendentals=rows * half
            ),
        )(layer_input, out_cotangent, gate_matrix, up_matrix, down_matrix)
        return copied(results)

    return on_device


def solution(mesh):
    return jax.shard_map(
        make(mesh.shape["fs"], mesh.shape["tp"]),
        mesh=mesh,
        in_specs=(P("fs", "tp"), P("fs", "tp"), P("fs", "tp"), P("fs", "tp"), P("tp", "fs")),
        out_specs=(P("fs", "tp"), P("fs", "tp"), P("fs", "tp"), P("tp", "fs")),
        check_vma=False,
    )
```

```python
import functools

import jax
import jax.numpy as jnp
from jax import lax
from jax.experimental import pallas as pl
from jax.experimental.pallas import tpu as pltpu
from jax.sharding import PartitionSpec as P

CORES = 2
TILE = 256
STRIPS = 3
HALVES = 2
PIECES = 3

NN = ((1,), (0,))
TN = ((0,), (0,))
NT = ((1,), (1,))

GATE, UP, DOWN = range(3)


def dot(left, right, dims):
    return lax.dot_general(left, right, (dims, ((), ())), preferred_element_type=jnp.float32)


def narrow(value):
    return value.astype(jnp.bfloat16)


def wide(value):
    return value.astype(jnp.float32)


def xor(left, right, n):
    total = 0
    k = 1
    while k < n:
        total = total + k * lax.rem(lax.div(left, k) + right // k % 2, 2)
        k *= 2
    return total


def kernel(
    n_fs,
    n_tp,
    layer_input,
    out_cotangent,
    gate_matrix,
    up_matrix,
    down_matrix,
    input_grad,
    gate_grad,
    up_grad,
    down_grad,
    xg,
    w,
    ab,
    delta,
    y_out,
    y_in,
    far_in,
    direct_in,
    near_in,
    core_in,
    dx_out,
    dx_core,
    dx_x,
    dx_z,
    local_sem,
    out_sem,
    ag_core,
    ag_near,
    ag_far,
    ag_direct,
    ag_y,
    tok_z,
    tok_x,
    tok_core,
    rs_y,
    rs_far,
    rs_direct,
    rs_near,
    rs_core,
    dx_core_sem,
    dx_x_sem,
    dx_z_sem,
):
    n_x = n_tp // CORES
    n_y = n_x
    n_z = n_fs // n_y
    per_quarter = n_fs // n_tp
    far = range(2, n_z, 2)
    tokens, part = layer_input.shape
    depth, width = gate_matrix.shape
    half = width // 2
    model = n_tp * part
    rows = 2 * tokens
    near = n_x * part

    fs = lax.axis_index("fs")
    tp = lax.axis_index("tp")
    z, y = lax.div(fs, n_y), lax.rem(fs, n_y)
    x, core = lax.div(tp, CORES), lax.rem(tp, CORES)
    mine = 1 - lax.rem(lax.rem(z, 2) + core, 2)

    def at_z(by):
        return {"fs": xor(z, by, n_z) * n_y + y}

    def at_y(by):
        return {"fs": z * n_y + xor(y, by, n_y)}

    def at_x(by):
        return {"tp": xor(x, by, n_x) * CORES + core}

    at_core = {"tp": x * CORES + 1 - core}

    def place(zr, yr):
        return xor(z, zr, n_z) * n_y + xor(y, yr, n_y)

    def first(where, tp_there=tp):
        quarter = lax.div(where, per_quarter)
        turned = 0
        k = 1
        while k < n_tp:
            turned = turned + k * lax.rem(lax.div(quarter, k) + lax.div(tp_there, k), 2)
            k *= 2
        slot = lax.rem(turned, CORES) * n_x + lax.div(turned, CORES)
        return slot * part + lax.rem(where, per_quarter) * depth

    def span(start, size):
        return pl.ds(pl.multiple_of(start, depth), size)

    def remote(src, dst, sems, index, device):
        return pltpu.make_async_remote_copy(
            src_ref=src,
            dst_ref=dst,
            send_sem=sems.at[(0, *index)],
            recv_sem=sems.at[(1, *index)],
            device_id=device,
            device_id_type=pl.DeviceIdType.MESH,
        )

    barrier = pltpu.get_barrier_semaphore()
    partners = (
        [at_core, at_z(1)]
        + [at_z(e) for e in far]
        + [at_z(3)]
        + [at_y(d) for d in range(1, n_y)]
        + [at_x(d) for d in range(1, n_x)]
    )
    for partner in partners:
        pl.semaphore_signal(
            barrier, inc=1, device_id=partner, device_id_type=pl.DeviceIdType.MESH
        )

    outer = lax.div(jnp.abs(2 * z - (n_z - 1)), n_z - 1)
    at_ends = pl.when(outer == 1)
    at_inner = pl.when(outer == 0)

    shards = (gate_matrix, up_matrix)
    sources = (layer_input, out_cotangent)
    here = first(fs)
    kept_row = mine * here + (1 - mine) * model
    sent_row = mine * first(fs, x * CORES + 1 - core) + (1 - mine) * model

    def load_down():
        return pltpu.make_async_copy(
            down_matrix, dx_core.at[pl.ds(0, width), pl.ds(0, depth)], local_sem.at[DOWN]
        )

    def turn_down():
        load_down().wait()
        w[DOWN, span(kept_row, depth), :] = dx_core[span(core * half, half), :depth].T
        y_out[DOWN, 0, 0] = dx_core[span((1 - core) * half, half), :depth].T

    def keep_shard(m):
        return pltpu.make_async_copy(
            shards[m].at[:, span(core * half, half)],
            w.at[m, span(kept_row, depth), :],
            local_sem.at[m],
        )

    def keep_tokens(k):
        return pltpu.make_async_copy(
            sources[k], xg.at[k, pl.ds(0, tokens), pl.ds(0, part)], local_sem.at[3 + k]
        )

    def swap_shard(m):
        if m == DOWN:
            src = y_out.at[DOWN, 0, 0]
        else:
            src = shards[m].at[:, span((1 - core) * half, half)]
        return remote(
            src,
            w.at[m, span(sent_row, depth), :],
            ag_core,
            (m,),
            at_core,
        )

    def near_shard(m):
        return remote(
            w.at[m, pl.ds(model, depth), :], w.at[m, span(here, depth), :], ag_near, (m,), at_z(1)
        )

    def direct_shard(m):
        return remote(
            w.at[m, pl.ds(model, depth), :], w.at[m, span(here, depth), :], ag_direct, (m,), at_z(3)
        )

    def far_shard(m, e, s):
        block = w.at[m, span(first(place(s, 0)), depth), :]
        return remote(block, block, ag_far, (m, e - 2 + s), at_z(e))

    def y_shard(m, zr, yr):
        block = w.at[m, span(first(place(zr, 0)), depth), :]
        return remote(block, block, ag_y, (m, zr, yr - 1), at_y(yr))

    piece = tokens // PIECES

    def token_z(k, h):
        return remote(
            sources[k].at[pl.ds(h * piece, piece), :],
            xg.at[k, pl.ds(tokens + h * piece, piece), pl.ds(0, part)],
            tok_z,
            (k, h),
            at_z(1),
        )

    def token_x(k, p, xr):
        here = pl.ds(tokens + (p - 1) * piece, piece) if p else pl.ds(0, tokens)
        src = xg.at[k, here, pl.ds(0, part)] if p else sources[k]
        dst = xg.at[k, here, pl.ds(xr * part, part)]
        return remote(src, dst, tok_x, (k, p, xr - 1), at_x(xr))

    def token_core(k, p):
        here = pl.ds(tokens + (p - 1) * piece, piece) if p else pl.ds(0, tokens)
        return remote(
            xg.at[k, here, pl.ds(0, near)],
            xg.at[k, here, pl.ds(near, near)],
            tok_core,
            (k, p),
            at_core,
        )

    def pass_tokens(k, h):
        token_z(k, h).wait_recv()
        for xr in range(1, n_x):
            token_x(k, 1 + h, xr).start()

    def join_tokens(k, p):
        if p == 0:
            keep_tokens(k).wait()
        for xr in range(1, n_x):
            token_x(k, p, xr).wait_recv()
        token_core(k, p).start()

    def await_tokens(k):
        for p in range(1 + PIECES):
            token_core(k, p).wait_recv()

    def relay_near(m):
        near_shard(m).wait_recv()

        @at_inner
        def _():
            far_shard(m, 2, 1).start()

        send_y_shards(m, 1)

    def relay_far(m):
        far_shard(m, 2, 0).wait_recv()
        send_y_shards(m, 2)

    def relay_last(m):
        @at_inner
        def _():
            direct_shard(m).wait_recv()

        @at_ends
        def _():
            far_shard(m, 2, 1).wait_recv()

        send_y_shards(m, 3)


    def send_y_shards(m, zr):
        for yr in range(1, n_y):
            y_shard(m, zr, yr).start()

    for m in (GATE, UP):
        keep_shard(m).start()
    load_down().start()
    for k in range(2):
        keep_tokens(k).start()
    pl.semaphore_wait(barrier, len(partners))

    for m in (GATE, UP):
        swap_shard(m).start()
    for k in range(2):
        for xr in range(1, n_x):
            token_x(k, 0, xr).start()
    for m in (GATE, UP):
        keep_shard(m).wait()
        swap_shard(m).wait_recv()
        near_shard(m).start()
        send_y_shards(m, 0)
    for h in range(PIECES):
        token_z(0, h).start()
    for m in (GATE, UP):
        far_shard(m, 2, 0).start()

    @at_ends
    def _():
        direct_in[...] = jnp.zeros_like(direct_in)
        far_in[:, 1] = jnp.zeros((3, depth, half), far_in.dtype)

    turn_down()
    swap_shard(DOWN).start()
    swap_shard(DOWN).wait_recv()
    send_y_shards(DOWN, 0)
    @at_inner
    def _():
        for m in (GATE, UP):
            relay_near(m)
        for m in (GATE, UP):
            direct_shard(m).start()
        for h in range(PIECES):
            token_z(1, h).start()
        near_shard(DOWN).start()
        for h in range(PIECES):
            pass_tokens(0, h)
        for m in (GATE, UP):
            relay_far(m)
        for p in range(1 + PIECES):
            join_tokens(0, p)
        far_shard(DOWN, 2, 0).start()
        for m in (GATE, UP):
            relay_last(m)
        relay_near(DOWN)
        direct_shard(DOWN).start()

    @at_ends
    def _():
        near_shard(DOWN).start()
        for h in range(PIECES):
            token_z(1, h).start()
        far_shard(DOWN, 2, 0).start()
        for m in (GATE, UP):
            relay_far(m)
        for m in (GATE, UP):
            relay_last(m)
        for m in (GATE, UP):
            relay_near(m)
        for h in range(PIECES):
            pass_tokens(0, h)
            join_tokens(0, h)
        join_tokens(0, PIECES)

    def arrived(m):
        for zr in range(n_z):
            for yr in range(1, n_y):
                y_shard(m, zr, yr).wait_recv()

    arrived(GATE)
    arrived(UP)
    await_tokens(0)

    def tile_of(i):
        return pl.ds(pl.multiple_of(i * TILE, TILE), TILE)

    strips = [slice(s * half // STRIPS, (s + 1) * half // STRIPS) for s in range(STRIPS)]

    def first_stage(begin, end):
        @pl.loop(begin, end)
        def _(i):
            tile = tile_of(i)
            mine_rows = xg[0, tile, :]
            for cols in strips:
                gate_pre = dot(mine_rows, w[GATE, :model, cols], NN)
                up_pre = dot(mine_rows, w[UP, :model, cols], NN)
                sigmoid_gate = jax.nn.sigmoid(gate_pre)
                activation = gate_pre * sigmoid_gate
                ab[0, tile, cols] = activation
                ab[1, tile, cols] = up_pre * sigmoid_gate * (1.0 + gate_pre * (1.0 - sigmoid_gate))
                delta[DOWN, tile, cols] = narrow(activation * up_pre)

    tiles = rows // TILE
    for h in range(PIECES):
        first_stage(h * tiles // PIECES, (h + 1) * tiles // PIECES)
        pass_tokens(1, h)
        join_tokens(1, h)
        if h == 0:
            relay_far(DOWN)
        elif h == 1:

            @at_ends
            def _():
                relay_last(DOWN)

    @at_ends
    def _():
        relay_near(DOWN)

    join_tokens(1, PIECES)

    @at_inner
    def _():
        relay_last(DOWN)

    await_tokens(1)

    def term(m, zr, yr):
        cols = span(first(place(zr, yr)), depth)
        pieces = [pl.ds(p * tokens, tokens) for p in range(2)]
        return sum(dot(xg[lax.div(m, 2), piece, cols], delta[m, piece, :], TN) for piece in pieces)

    def y_term(m, zr, yr):
        return remote(
            y_out.at[m, zr, yr - 1], y_in.at[m, zr, yr - 1], rs_y, (m, zr, yr - 1), at_y(yr)
        )

    def far_sum(m, zr, e):
        return remote(y_out.at[m, zr, 0], far_in.at[m, zr - 2], rs_far, (m, zr - 2), at_z(e))

    def direct_sum(m):
        return remote(y_out.at[m, 3, 0], direct_in.at[m], rs_direct, (m,), at_z(3))

    def near_sum(m):
        return remote(y_out.at[m, 1, 0], near_in.at[m], rs_near, (m,), at_z(1))

    def core_sum(m):
        return remote(y_out.at[m, 0, 0], core_in.at[m], rs_core, (m,), at_core)

    def send_y(m, zr):
        for yr in range(1, n_y):
            y_out[m, zr, yr - 1] = narrow(term(m, zr, yr))
            y_term(m, zr, yr).start()

    def y_sum(m, zr):
        total = term(m, zr, 0)
        for yr in range(1, n_y):
            y_term(m, zr, yr).wait_recv()
            total = total + wide(y_in[m, zr, yr - 1])
        y_term(m, zr, 1).wait_send()
        return total

    def cross(m, zr, e):
        y_out[m, zr, 0] = narrow(y_sum(m, zr))
        if zr != 3:
            far_sum(m, zr, e).start()
            return

        @at_inner
        def _():
            direct_sum(m).start()

        @at_ends
        def _():
            far_sum(m, 3, 2).start()

    def pair(m):
        total = y_sum(m, 1)

        @at_inner
        def _():
            far_sum(m, 3, 2).wait_recv()

        y_out[m, 1, 0] = narrow(total + wide(far_in[m, 1]))
        near_sum(m).start()

    def own_stage(m):
        return pl.ds(pl.multiple_of((2 * m + core) * depth, depth), depth)

    def other_stage(m):
        return pl.ds(pl.multiple_of((2 * m + 1 - core) * depth, depth), depth)

    def own(m):
        total = y_sum(m, 0)
        for e in far:
            far_sum(m, e, e).wait_recv()
            total = total + wide(far_in[m, e - 2])
        near_sum(m).wait_recv()

        @at_inner
        def _():
            direct_sum(m).wait_recv()

        other = wide(near_in[m]) + wide(direct_in[m])
        y_out[m, 0, 0] = narrow(jnp.where(mine == 1, other, total))
        core_sum(m).start()
        kept = jnp.where(mine == 1, total, other)
        if m is DOWN:
            ab[1, span(core * half, half), :depth] = kept.T
        else:
            ab[0, own_stage(m), :] = kept

    def put(m):
        if m == DOWN:
            stage = ab.at[1, pl.ds(0, width), pl.ds(0, depth)]
            return [pltpu.make_async_copy(stage, down_grad, out_sem.at[DOWN, 0])]
        out = (gate_grad, up_grad)[m]
        return [
            pltpu.make_async_copy(
                ab.at[0, pl.ds((2 * m + p) * depth, depth), :],
                out.at[:, pl.ds(p * half, half)],
                out_sem.at[m, p],
            )
            for p in range(2)
        ]

    def finish(m):
        core_sum(m).wait_recv()
        if m == DOWN:
            ab[1, span((1 - core) * half, half), :depth] = wide(core_in[m]).T
        else:
            ab[0, other_stage(m), :] = wide(core_in[m])
        for copy in put(m):
            copy.start()

    @pl.loop(0, 3)
    def _(i):
        send_y(DOWN, 3 - i)

    arrived(DOWN)

    def second_stage(begin, end):
        @pl.loop(begin, end)
        def _(i):
            tile = tile_of(i)
            mine_rows = xg[1, tile, :]
            for cols in strips:
                hidden_delta = dot(mine_rows, w[DOWN, :model, cols], NN)
                delta[UP, tile, cols] = narrow(hidden_delta * ab[0, tile, cols])
                delta[GATE, tile, cols] = narrow(hidden_delta * ab[1, tile, cols])

    second_stage(0, tiles)

    def dx_tile(tile, begin):
        total = dot(delta[GATE, tile, :], w[GATE, begin : begin + part, :], NT)
        return total + dot(delta[UP, tile, :], w[UP, begin : begin + part, :], NT)

    def dx_rows(p):
        return pl.ds(p * tokens, tokens)

    def dx_swap(p):
        here = dx_rows(p)
        return remote(dx_out.at[here, :], dx_core.at[here, :], dx_core_sem, (p,), at_core)

    def dx_over_x(p, xr):
        here = dx_rows(p)
        return remote(
            dx_core.at[here, pl.ds(xr * part, part)],
            dx_x.at[xr - 1, here, :],
            dx_x_sem,
            (p, xr - 1),
            at_x(xr),
        )

    dx_over_z = remote(
        dx_core.at[pl.ds(tokens, tokens), pl.ds(0, part)], dx_z, dx_z_sem, (), at_z(1)
    )

    def dx_tiles(p):
        return pl.loop(p * tiles // 2, (p + 1) * tiles // 2)

    def dx_give(p):
        @dx_tiles(p)
        def _(i):
            tile = tile_of(i)
            for xr in range(n_x):
                cols = pl.ds(xr * part, part)
                dx_out[tile, cols] = narrow(dx_tile(tile, near + xr * part))

        dx_swap(p).start()

    def dx_take(p):
        dx_swap(p).wait_recv()

        @dx_tiles(p)
        def _(i):
            tile = tile_of(i)
            for xr in range(n_x):
                cols = pl.ds(xr * part, part)
                dx_core[tile, cols] = narrow(dx_tile(tile, xr * part) + wide(dx_core[tile, cols]))

        for xr in range(1, n_x):
            dx_over_x(p, xr).start()

    def dx_sum(p):
        for xr in range(1, n_x):
            dx_over_x(p, xr).wait_recv()

        @dx_tiles(p)
        def _(i):
            tile = tile_of(i)
            total = wide(dx_core[tile, pl.ds(0, part)])
            for xr in range(1, n_x):
                total = total + wide(dx_x[xr - 1, tile, :])
            dx_core[tile, pl.ds(0, part)] = narrow(total)

    def send_pair(zr):
        @pl.loop(0, 2)
        def _(m):
            send_y(m, zr)

    dx_give(1)
    cross(DOWN, 3, 2)
    send_pair(3)
    cross(DOWN, 2, 2)
    dx_take(1)
    pair(DOWN)
    send_y(GATE, 1)
    dx_give(0)
    cross(GATE, 3, 2)
    send_y(UP, 1)
    dx_take(0)
    cross(UP, 3, 2)
    send_pair(2)
    dx_sum(1)
    dx_over_z.start()
    pair(GATE)
    swap_shard(DOWN).wait_send()
    send_y(DOWN, 0)
    send_y(GATE, 0)
    pair(UP)
    send_y(UP, 0)

    @pl.loop(0, 2)
    def _(m):
        cross(m, 2, 2)

    dx_sum(0)
    dx_over_z.wait_recv()

    @pl.loop(0, tokens // TILE)
    def _(i):
        tile = tile_of(i)
        dx_z[tile, :] = narrow(wide(dx_core[tile, pl.ds(0, part)]) + wide(dx_z[tile, :]))

    put_dx = pltpu.make_async_copy(dx_z, input_grad, local_sem.at[5])
    put_dx.start()
    own(DOWN)
    finish(DOWN)

    for m in (GATE, UP):
        own(m)
        finish(m)

    dx_over_z.wait_send()
    for p in range(2):
        dx_swap(p).wait_send()
        for xr in range(1, n_x):
            dx_over_x(p, xr).wait_send()
    for k in range(2):
        for h in range(PIECES):
            token_z(k, h).wait_send()
        for p in range(1 + PIECES):
            token_core(k, p).wait_send()
            for xr in range(1, n_x):
                token_x(k, p, xr).wait_send()
    for m in range(3):
        if m != DOWN:
            swap_shard(m).wait_send()
        near_shard(m).wait_send()
        near_sum(m).wait_send()
        core_sum(m).wait_send()
        far_shard(m, 2, 0).wait_send()
        far_sum(m, 2, 2).wait_send()

        @at_inner
        def _():
            far_shard(m, 2, 1).wait_send()
            direct_shard(m).wait_send()
            direct_sum(m).wait_send()

        @at_ends
        def _():
            far_sum(m, 3, 2).wait_send()

        for zr in range(n_z):
            for yr in range(1, n_y):
                y_shard(m, zr, yr).wait_send()
                if yr > 1:
                    y_term(m, zr, yr).wait_send()
        for copy in put(m):
            copy.wait()
    put_dx.wait()


def hand_over(*refs):
    count = (len(refs) - 2) // 3
    sources, results, stages = refs[:count], refs[count : 2 * count], refs[2 * count : 3 * count]
    came, went = refs[3 * count :]

    def piece(ref, p):
        size = ref.shape[0] // HALVES
        return ref.at[pl.ds(p * size, size), :]

    def load(i, p):
        return pltpu.make_async_copy(piece(sources[i], p), piece(stages[i], p), came.at[i, p])

    def store(i, p):
        return pltpu.make_async_copy(piece(stages[i], p), piece(results[i], p), went.at[i, p])

    order = [(i, p) for i in range(count) for p in range(HALVES)]
    for i, p in order:
        load(i, p).start()
    for i, p in order:
        load(i, p).wait()
        store(i, p).start()
    for i, p in order:
        store(i, p).wait()


def copied(results):
    shapes = tuple(jax.ShapeDtypeStruct(r.shape, r.dtype) for r in results)
    any_space = pl.BlockSpec(memory_space=pl.ANY)
    sems = pltpu.SemaphoreType.DMA((len(results), HALVES))
    return pl.pallas_call(
        hand_over,
        out_shape=shapes,
        in_specs=[any_space] * len(results),
        out_specs=(any_space,) * len(results),
        scratch_shapes=[pltpu.VMEM(r.shape, r.dtype) for r in results] + [sems, sems],
    )(*results)


def make(n_fs, n_tp):
    n_x = n_tp // CORES
    n_y = n_x
    n_z = n_fs // n_y

    def on_device(layer_input, out_cotangent, gate_matrix, up_matrix, down_matrix):
        tokens, part = layer_input.shape
        depth, width = gate_matrix.shape
        half = width // 2
        model = n_tp * part
        rows = 2 * tokens
        near = n_x * part
        bf16, f32 = jnp.bfloat16, jnp.float32
        sem = pltpu.SemaphoreType.DMA
        any_space = pl.BlockSpec(memory_space=pl.ANY)
        wide_grad = jax.ShapeDtypeStruct((depth, width), f32)
        flops = 2 * 8 * rows * half * model
        results = pl.pallas_call(
            functools.partial(kernel, n_fs, n_tp),
            out_shape=(
                jax.ShapeDtypeStruct((tokens, part), bf16),
                wide_grad,
                wide_grad,
                jax.ShapeDtypeStruct((width, depth), f32),
            ),
            in_specs=[any_space] * 5,
            out_specs=(any_space,) * 4,
            scratch_shapes=[
                pltpu.VMEM((2, rows, model), bf16),
                pltpu.VMEM((3, model + depth, half), bf16),
                pltpu.VMEM((2, rows, half), f32),
                pltpu.VMEM((3, rows, half), bf16),
                pltpu.VMEM((3, n_z, n_y - 1, depth, half), bf16),
                pltpu.VMEM((3, n_z, n_y - 1, depth, half), bf16),
                pltpu.VMEM((3, n_z - 2, depth, half), bf16),
                pltpu.VMEM((3, depth, half), bf16),
                pltpu.VMEM((3, depth, half), bf16),
                pltpu.VMEM((3, depth, half), bf16),
                pltpu.VMEM((rows, near), bf16),
                pltpu.VMEM((rows, near), bf16),
                pltpu.VMEM((n_x - 1, rows, part), bf16),
                pltpu.VMEM((tokens, part), bf16),
                sem((6,)),
                sem((3, 2)),
                sem((2, 3)),
                sem((2, 3)),
                sem((2, 3, n_z - 2)),
                sem((2, 3)),
                sem((2, 3, n_z, n_y - 1)),
                sem((2, 2, PIECES)),
                sem((2, 2, 1 + PIECES, n_x - 1)),
                sem((2, 2, 1 + PIECES)),
                sem((2, 3, n_z, n_y - 1)),
                sem((2, 3, n_z - 2)),
                sem((2, 3)),
                sem((2, 3)),
                sem((2, 3)),
                sem((2, 2)),
                sem((2, 2, n_x - 1)),
                sem((2,)),
            ],
            compiler_params=pltpu.CompilerParams(
                collective_id=0, has_side_effects=True, vmem_limit_bytes=67043328
            ),
            cost_estimate=pl.CostEstimate(
                flops=flops, bytes_accessed=rows * model, transcendentals=rows * half
            ),
        )(layer_input, out_cotangent, gate_matrix, up_matrix, down_matrix)
        return copied(results)

    return on_device


def solution(mesh):
    return jax.shard_map(
        make(mesh.shape["fs"], mesh.shape["tp"]),
        mesh=mesh,
        in_specs=(P("fs", "tp"), P("fs", "tp"), P("fs", "tp"), P("fs", "tp"), P("tp", "fs")),
        out_specs=(P("fs", "tp"), P("fs", "tp"), P("fs", "tp"), P("tp", "fs")),
        check_vma=False,
    )
```
